768 devices in a mesh: kv: 192 (over z, y, core), tp: 4 (over x).
Axes of the slice: x: 4, y: 8, z: 12, core: 2. Of those that a mesh axis runs over, the one named last changes fastest.
Arguments:
- queries: bfloat16 [49152, 3072], P('kv', 'tp'), may hold values from -6 to 6
- keys: bfloat16 [49152, 512], P('kv', 'tp'), may hold values from -6 to 6
- values: bfloat16 [49152, 512], P('kv', 'tp'), may hold values from -6 to 6
- log_sums: float32 [24, 49152], P('tp', 'kv'), may hold values from 6 to 7.5
- out_grad: bfloat16 [49152, 3072], P('kv', 'tp'), may hold values from -6 to 6
- chosen: int32 [768, 4, 8], P('kv', 'tp'), may hold values from 0 to 767, as said below
- inputs: bfloat16 [49152, 3072], P('kv', 'tp'), may hold values from -6 to 6
Outputs:
- query_grad: bfloat16 [49152, 3072], P('kv', 'tp')
- key_grad: bfloat16 [49152, 512], P('kv', 'tp')
- value_grad: bfloat16 [49152, 512], P('kv', 'tp')
- weight_grad: float32 [3072, 512], P('kv', 'tp')
The draws below stay inside these ranges and needn't reach their ends.
Inputs may be any that keep to these rules, and one draw needn't show every extreme that they name: `chosen`: for query block g and key head h, every slot holds g (an empty slot) or a key block c with g - 16 <= c < g; the blocks of the live slots of one list are distinct; each list has between 4 and 8 live slots, except that query block g has at most g of them (block 0 has none).
All inputs are finite; a program needn't handle non-finite values.
Results may differ from the reference program's by a relative error of at most 0.0049.
Values may be sent and summed in bfloat16 or wider, within the bound.
A program may use at most 32 MiB of HBM per device.

```python
import jax
import jax.numpy as jnp
from jax import lax

D = 3072
HDIM = 128
QPK = 6
BLK = 64
SEL = 8
REACH = 4
BPD = 4
KVH = 4
HEADS = 24
NBLK = 768
TOKENS = 49152


def draw_chosen(key, part):
    window_span = REACH * BPD
    order_key = jax.random.fold_in(key, 11)
    count_key = jax.random.fold_in(key, 12)
    blocks = jnp.arange(NBLK, dtype=jnp.int32)[:, None, None]
    offsets = jnp.arange(1, window_span + 1, dtype=jnp.int32)[None, None, :]
    scores = jax.random.randint(order_key, (NBLK, KVH, window_span), 0, 1 << 20, dtype=jnp.int32) * window_span + offsets - 1
    scores = jnp.where(blocks - offsets >= 0, scores, -offsets)
    top_values, picked = lax.top_k(scores, SEL)
    chosen_ids = blocks - 1 - picked.astype(jnp.int32)
    live_count = jax.random.randint(count_key, (NBLK, KVH, 1), SEL // 2, SEL + 1, dtype=jnp.int32)
    slot_index = jnp.arange(SEL, dtype=jnp.int32)[None, None, :]
    keep_mask = (slot_index < live_count) & (chosen_ids >= 0)
    return jnp.where(keep_mask, chosen_ids, blocks)


def steps_of(stream_key, shape, shards, least, largest):
    factor_of = 1.0
    for dim, parts in shards:
        steps = jax.random.uniform(jax.random.fold_in(jax.random.fold_in(stream_key, 6), dim), (parts,), jnp.float32, least / len(shards), largest / len(shards))
        factor_of = factor_of * jnp.repeat(jnp.exp(steps), shape[dim] // parts).reshape((-1,) + (1,) * (len(shape) - 1 - dim))
    return factor_of


def gaussian(stream_key, shape, width, reach, split=(), kind=jnp.bfloat16):
    level = steps_of(stream_key, shape, split, -0.22, 0.18) if split else 1.0
    entries = jax.random.normal(stream_key, shape, jnp.float32) * width * level
    return jnp.minimum(jnp.maximum(entries, -reach), reach).astype(kind)


def setup_inputs(seed: int = 0) -> dict:
    splits = jax.random.split(jax.random.key(seed), 8)
    queries = gaussian(splits[0], (TOKENS, HEADS * HDIM), 1.0, 6.0, ((0, 192), (1, 4)))
    keys = gaussian(splits[1], (TOKENS, KVH * HDIM), 1.0, 6.0, ((0, 192), (1, 4)))
    values = gaussian(splits[2], (TOKENS, KVH * HDIM), 1.0, 6.0, ((0, 192), (1, 4)))
    log_sums = jnp.clip(6.0 + 1.5 * jax.random.uniform(splits[3], (HEADS, TOKENS), jnp.float32) ** steps_of(splits[3], (HEADS, TOKENS), ((0, 4), (1, 192)), -0.2, 0.2), 6.0, 7.5)
    out_grad = gaussian(splits[4], (TOKENS, HEADS * HDIM), 1.0, 6.0, ((0, 192), (1, 4)))
    chosen = draw_chosen(jax.random.fold_in(splits[7], 71), 0)
    inputs = gaussian(splits[6], (TOKENS, D), 1.0, 6.0, ((0, 192), (1, 4)))
    return {"queries": queries, "keys": keys, "values": values, "log_sums": log_sums, "out_grad": out_grad, "chosen": chosen, "inputs": inputs}


def rounded(tensor):
    return lax.optimization_barrier(tensor.astype(jnp.bfloat16)).astype(jnp.float32)


def reference(queries, keys, values, log_sums, out_grad, chosen, inputs):
    scaling = HDIM ** -0.5
    query_tile_set = queries.reshape(NBLK, BLK, KVH, QPK, HDIM)
    gradient_tiles = out_grad.reshape(NBLK, BLK, KVH, QPK, HDIM)
    sum_tiles = log_sums.reshape(KVH, QPK, NBLK, BLK).transpose(2, 0, 1, 3)
    key_tiles = keys.reshape(NBLK, BLK, KVH, HDIM)
    value_tiles = values.reshape(NBLK, BLK, KVH, HDIM)
    head_ids = jnp.arange(KVH, dtype=jnp.int32)[:, None]
    offsets = jnp.arange(BLK, dtype=jnp.int32)
    causal = (offsets[None, :] <= offsets[:, None])[None, :, None, :]

    def visit(carry, index):
        key_acc, value_acc = carry
        listed = chosen[index]
        live_slots = listed < index
        sel_keys = key_tiles[listed, :, head_ids]
        sel_values = value_tiles[listed, :, head_ids]
        own_keys = lax.dynamic_index_in_dim(key_tiles, index, 0, keepdims=False).transpose(1, 0, 2)[:, None]
        own_values = lax.dynamic_index_in_dim(value_tiles, index, 0, keepdims=False).transpose(1, 0, 2)[:, None]
        all_keys = jnp.concatenate([sel_keys, own_keys], 1).reshape(KVH, (SEL + 1) * BLK, HDIM).astype(jnp.float32)
        all_values = jnp.concatenate([sel_values, own_values], 1).reshape(KVH, (SEL + 1) * BLK, HDIM).astype(jnp.float32)
        mask_sel = jnp.broadcast_to(live_slots[:, None, :, None], (KVH, BLK, SEL, BLK))
        mask_own = jnp.broadcast_to(causal, (KVH, BLK, 1, BLK))
        permitted_mask = jnp.concatenate([mask_sel, mask_own], 2).reshape(KVH, BLK, (SEL + 1) * BLK)
        query_rows = lax.dynamic_index_in_dim(query_tile_set, index, 0, keepdims=False).astype(jnp.float32)
        grad_rows = lax.dynamic_index_in_dim(gradient_tiles, index, 0, keepdims=False).astype(jnp.float32)
        sum_rows = lax.dynamic_index_in_dim(sum_tiles, index, 0, keepdims=False)
        scores = jnp.einsum('qhgd,hkd->hgqk', query_rows, all_keys) * scaling
        weights = jnp.where(permitted_mask[:, None], jnp.exp(scores - sum_rows[..., None]), 0.0)
        grad_weights = jnp.einsum('qhgd,hkd->hgqk', grad_rows, all_values)
        delta_rows = jnp.sum(weights * grad_weights, -1, keepdims=True)
        score_gradient = rounded(weights * (grad_weights - delta_rows))
        weights_reduced = rounded(weights)
        query_part = jnp.einsum('hgqk,hkd->qhgd', score_gradient, all_keys) * scaling
        key_part = (jnp.einsum('hgqk,qhgd->hkd', score_gradient, query_rows) * scaling).reshape(KVH, SEL + 1, BLK, HDIM)
        value_part = jnp.einsum('hgqk,qhgd->hkd', weights_reduced, grad_rows).reshape(KVH, SEL + 1, BLK, HDIM)
        key_acc = key_acc.at[listed, :, head_ids].add(key_part[:, :SEL])
        key_acc = key_acc.at[index].add(key_part[:, SEL].transpose(1, 0, 2))
        value_acc = value_acc.at[listed, :, head_ids].add(value_part[:, :SEL])
        value_acc = value_acc.at[index].add(value_part[:, SEL].transpose(1, 0, 2))
        return (key_acc, value_acc), query_part.reshape(BLK, HEADS * HDIM).astype(jnp.bfloat16)

    zeros_acc = jnp.zeros((NBLK, BLK, KVH, HDIM), jnp.float32)
    (key_acc, value_acc), query_blocks = lax.scan(visit, (zeros_acc, zeros_acc), jnp.arange(NBLK, dtype=jnp.int32))
    query_grad = query_blocks.reshape(TOKENS, HEADS * HDIM)
    key_grad = key_acc.reshape(TOKENS, KVH * HDIM).astype(jnp.bfloat16)
    value_grad = value_acc.reshape(TOKENS, KVH * HDIM).astype(jnp.bfloat16)
    weight_grad = jnp.dot(inputs.T, value_grad, preferred_element_type=jnp.float32)
    return (query_grad, key_grad, value_grad, weight_grad)
```

```python
import functools

import jax
import jax.numpy as jnp
from jax import lax
from jax.experimental import pallas as pl
from jax.experimental.pallas import tpu as pltpu
from jax.sharding import PartitionSpec as P

MESH = pl.DeviceIdType.MESH
LOG2E = 1.4426950408889634
MASKED = -1e30

NX, NY, NZ = 4, 8, 12
NCHIP = NY * NZ
T = 256
HD = 128
G = 6
BL = 64
NB = 4
SELS = 8
CPX = NCHIP // NX
RW = 16
HR = CPX * RW

NN = (((1,), (0,)), ((), ()))
NT = (((1,), (1,)), ((), ()))
TN = (((0,), (0,)), ((), ()))


def mm(a, b, dims):
    return lax.dot_general(a, b, dims, preferred_element_type=jnp.float32)


def kernel(
    q_hbm, k_hbm, v_hbm, lse_hbm, do_hbm, ch_ref, in_hbm,
    dq_hbm, dk_hbm, dv_hbm, dw_hbm,
    q6, do6, in6, lse, kbuf, vbuf, hitb, ownb, pst, dpst, dvacc, dkacc, dqst,
    hs, ing, sxv, rxv, sretv, rretv, sxk, rxk, sretk, rretk, vg, kg,
    wpart, r1z, r1y, s1z, s1y, r2z, r2y, dwst,
    lsem, ssem, k_rs, v_rs, in_rs, x_rs, ret_rs, vg_rs, z_rs, y_rs, zs_s, ys_s, osem,
):
    kv = lax.axis_index("kv")
    x = lax.axis_index("tp")
    p = kv // 2
    c = kv % 2
    z = p // NY
    y = p % NY
    o = 1 - c

    def chip(step):
        return lax.rem(p + step + NCHIP, NCHIP)

    def at(chip_id, core):
        return (chip_id * 2 + core, x)

    partner = at(p, o)
    nxt, nxt2, prv, prv2 = (at(chip(s), c) for s in (1, 2, -1, -2))
    xr, xl = lax.rem(x + 1, NX), lax.rem(x + NX - 1, NX)

    barrier = pltpu.get_barrier_semaphore()
    peers = [partner, nxt, nxt2, prv, prv2]
    peers += [(p * 2 + d, xx) for xx in (xr, xl) for d in (0, 1)]
    for d in range(1, NZ):
        peers.append(at(lax.rem(z + d, NZ) * NY + y, c))
    for d in range(1, NY):
        peers.append(at(z * NY + lax.rem(y + d, NY), c))
    for peer in peers:
        pl.semaphore_signal(barrier, inc=1, device_id=peer, device_id_type=MESH)

    loads = []

    def load(src, dst, n):
        copy = pltpu.make_async_copy(src, dst, lsem.at[n])
        copy.start()
        return copy

    ld_k = load(k_hbm, kbuf.at[4 + c], 0)
    ld_q = [load(q_hbm.at[:, pl.ds(HD * h, HD)], q6.at[h], 1 + h) for h in range(G)]
    ld_l = load(lse_hbm, lse, 7)
    ld_v = load(v_hbm, vbuf.at[4 + c], 8)
    ld_i = [load(in_hbm.at[:, pl.ds(HD * h, HD)], in6.at[h], 9 + h) for h in range(G)]
    ld_d = [load(do_hbm.at[:, pl.ds(HD * h, HD)], do6.at[h], 15 + h) for h in range(G)]

    base = (p - 2) * 4 * 2 + 4 * c
    own0 = kv * NB
    wid = lax.broadcasted_iota(jnp.int32, (24, T), 0)
    lane = lax.broadcasted_iota(jnp.int32, (24, T), 1)
    hit = jnp.zeros((24, T), jnp.float32)
    for b in range(NB):
        in_b = (lane // BL) == b
        for k in range(SELS):
            named = ch_ref[b, 0, k]
            slot = jnp.where(named < own0 + b, named - base, -1)
            hit = jnp.where(in_b & (wid == slot), 1.0, hit)
    hitb[...] = jnp.where(hit > 0.5, 0.0, MASKED)
    krow = lax.broadcasted_iota(jnp.int32, (BL, T), 0)
    qlane = lax.broadcasted_iota(jnp.int32, (BL, T), 1)
    for j in range(NB):
        here = (qlane // BL) == j
        causal = here & (krow <= qlane - BL * j)
        ownb[j] = jnp.where(causal, 0.0, jnp.where(here, MASKED, hitb[16 + j : 17 + j, :]))

    for j in range(G):
        ld_i[j].wait()
        xt = in6[j].T
        for m in range(4):
            for d in range(2):
                r0 = (4 * j + m) * RW
                hs[d, r0 : r0 + RW, :] = xt[32 * m + 16 * d : 32 * m + 16 * d + 16, :]

    ld_k.wait()
    ld_v.wait()

    sends = []

    def send(src, dst, recv, device):
        n = len(sends)
        copy = pltpu.make_async_remote_copy(
            src_ref=src, dst_ref=dst, send_sem=ssem.at[n], recv_sem=recv,
            device_id=device, device_id_type=MESH,
        )
        copy.start()
        sends.append(copy)
        return copy

    def arrived(dst, recv):
        pltpu.make_async_copy(dst, dst, recv).wait()

    pl.semaphore_wait(barrier, len(peers))

    def kv_send(buf, rs, slot, device):
        send(buf.at[slot], buf.at[slot], rs.at[slot], device)

    def kv_send_to(buf, rs, src_slot, dst_slot, device):
        send(buf.at[src_slot], buf.at[dst_slot], rs.at[dst_slot], device)

    kv_send_to(kbuf, k_rs, 4 + c, 2 + c, nxt)
    kv_send(kbuf, k_rs, 4 + c, partner)
    kv_send_to(vbuf, v_rs, 4 + c, 2 + c, nxt)
    kv_send(vbuf, v_rs, 4 + c, partner)
    send(hs.at[o], ing.at[0, c], in_rs.at[0, c], partner)
    for d in (0, 1):
        send(hs.at[d], ing.at[3, c], in_rs.at[3, c], (p * 2 + d, xr))
        send(hs.at[d], ing.at[1, c], in_rs.at[1, c], (p * 2 + d, xl))

    for copy in ld_q:
        copy.wait()
    ld_l.wait()
    for copy in ld_d:
        copy.wait()

    lse[...] = lse[...] * LOG2E
    factor = HD ** (-0.5) * LOG2E

    def value_terms(s):
        dvacc[s] = jnp.zeros((T, HD), jnp.float32)

        @pl.loop(0, G)
        def _(h):
            scores = mm(kbuf[s + c], q6[h], NT)
            row = lse[pl.ds(h, 1), :]
            for j in range(NB):
                part = scores[BL * j : BL * j + BL, :] * factor
                if s == 4:
                    shift = ownb[j] - row
                else:
                    shift = hitb[4 * s + j : 4 * s + j + 1, :] - row
                pst[s, h, BL * j : BL * j + BL, :] = jnp.exp2(part + shift)
            dvacc[s] += mm(pst[s, h].astype(jnp.bfloat16), do6[h], NN)

    value_terms(4)
    arrived(kbuf.at[2 + c], k_rs.at[2 + c])
    kv_send(kbuf, k_rs, 2 + c, partner)
    kv_send_to(kbuf, k_rs, 2 + c, c, nxt)
    value_terms(2)
    arrived(vbuf.at[2 + c], v_rs.at[2 + c])
    kv_send(vbuf, v_rs, 2 + c, partner)
    kv_send_to(vbuf, v_rs, 2 + c, c, nxt)
    arrived(kbuf.at[2 + o], k_rs.at[2 + o])
    arrived(kbuf.at[4 + o], k_rs.at[4 + o])
    value_terms(3)
    arrived(kbuf.at[c], k_rs.at[c])
    kv_send(kbuf, k_rs, c, partner)
    value_terms(0)
    arrived(kbuf.at[o], k_rs.at[o])
    value_terms(1)

    sxv[0] = dvacc[1].astype(jnp.bfloat16)
    sxv[1] = dvacc[3].astype(jnp.bfloat16)
    send(sxv, rxv, x_rs.at[0], partner)

    for d in (0, 1):
        arrived(ing.at[3, d], in_rs.at[3, d])
        arrived(ing.at[1, d], in_rs.at[1, d])
    send(ing.at[3, 0], ing.at[2, 0], in_rs.at[2, 0], (kv, xr))
    send(ing.at[1, 1], ing.at[2, 1], in_rs.at[2, 1], (kv, xl))
    arrived(vbuf.at[c], v_rs.at[c])
    kv_send(vbuf, v_rs, c, partner)

    arrived(rxv, x_rs.at[0])
    for k in range(2):
        dvacc[2 * k + 2 * o] += rxv[k].astype(jnp.float32)
    sretv[0] = dvacc[0].astype(jnp.bfloat16)
    sretv[1] = dvacc[2].astype(jnp.bfloat16)
    send(sretv.at[0], rretv.at[0], ret_rs.at[0], prv2)
    send(sretv.at[1], rretv.at[1], ret_rs.at[1], prv)

    for slot in (2 + o, 4 + o, o):
        arrived(vbuf.at[slot], v_rs.at[slot])
    for s in range(5):
        dkacc[s] = jnp.zeros((T, HD), jnp.float32)

    def score_terms(first, last):
        @pl.loop(first, last)
        def _(h):
            delta = jnp.zeros((1, T), jnp.float32)
            for s in range(5):
                dp = mm(vbuf[s + c], do6[h], NT)
                dpst[s] = dp
                delta = delta + jnp.sum(pst[s, h] * dp, axis=0, keepdims=True)
            dqt = jnp.zeros((HD, T), jnp.float32)
            for s in range(5):
                ds = (pst[s, h] * (dpst[s] - delta)).astype(jnp.bfloat16)
                dkacc[s] += mm(ds, q6[h], NN)
                dqt = dqt + mm(kbuf[s + c], ds, TN)
            dqst[h] = (dqt * HD ** (-0.5)).T.astype(jnp.bfloat16)

    score_terms(0, G)

    sxk[0] = dkacc[1].astype(jnp.bfloat16)
    sxk[1] = dkacc[3].astype(jnp.bfloat16)
    send(sxk, rxk, x_rs.at[1], partner)

    for k in range(2):
        arrived(rretv.at[k], ret_rs.at[k])
    total = dvacc[4] + rretv[0].astype(jnp.float32) + rretv[1].astype(jnp.float32)
    vg[c] = total.astype(jnp.bfloat16)
    send(vg.at[c], vg.at[c], vg_rs, partner)

    outs = []

    def store(src, dst):
        copy = pltpu.make_async_copy(src, dst, osem.at[len(outs)])
        copy.start()
        outs.append(copy)

    store(vg.at[c], dv_hbm)
    for h in range(G):
        store(dqst.at[h], dq_hbm.at[:, pl.ds(HD * h, HD)])

    arrived(ing.at[0, o], in_rs.at[0, o])
    for d in (0, 1):
        arrived(ing.at[2, d], in_rs.at[2, d])
    arrived(vg.at[o], vg_rs)

    for rel in range(4):
        if rel == 0:
            rows = mm(hs[c], vg[c], NN) + mm(ing[0, o], vg[o], NN)
        else:
            rows = mm(ing[rel, 0], vg[0], NN) + mm(ing[rel, 1], vg[1], NN)
        first = lax.rem(x + rel, NX) * CPX
        if rel == 0:
            first = x * CPX
        tiles = rows.astype(jnp.bfloat16).reshape(CPX, RW, HD)
        for a in range(CPX // NY):
            wpart[lax.div(first, NY) + a] = tiles[a * NY : (a + 1) * NY]

    def fan(n, src, dst, recv, sem, device, start=True):
        copies = []
        for d in range(1, n):
            copy = pltpu.make_async_remote_copy(
                src_ref=src(d), dst_ref=dst.at[d], send_sem=sem.at[d], recv_sem=recv.at[d],
                device_id=device(d), device_id_type=MESH,
            )
            if start:
                copy.start()
            copies.append(copy)
        return copies

    def total_of(n, own, got, recv):
        acc = own.astype(jnp.float32)
        for d in range(1, n):
            arrived(got.at[d], recv.at[d])
            acc = acc + got[d].astype(jnp.float32)
        return acc

    def z_at(d):
        return lax.rem(z + d, NZ)

    def y_at(d):
        return lax.rem(y + d, NY)

    def z_dev(d):
        return at(z_at(d) * NY + y, c)

    def y_dev(d):
        return at(z * NY + y_at(d), c)

    def first_z(start):
        return fan(NZ, lambda d: wpart.at[z_at(d)], r1z, z_rs, zs_s, z_dev, start)

    def first_y(start):
        return fan(NY, lambda d: wpart.at[:, y_at(d)], r1y, y_rs, ys_s, y_dev, start)

    @pl.when(c == 0)
    def _():
        first_z(True)

    @pl.when(c == 1)
    def _():
        first_y(True)

    arrived(rxk, x_rs.at[1])
    for k in range(2):
        dkacc[2 * k + 2 * o] += rxk[k].astype(jnp.float32)
    sretk[0] = dkacc[0].astype(jnp.bfloat16)
    sretk[1] = dkacc[2].astype(jnp.bfloat16)
    send(sretk.at[0], rretk.at[0], ret_rs.at[2], prv2)
    send(sretk.at[1], rretk.at[1], ret_rs.at[3], prv)

    @pl.when(c == 0)
    def _():
        acc = total_of(NZ, wpart[z], r1z, z_rs)
        s1z[...] = acc.astype(jnp.bfloat16)
        second = fan(NY, lambda d: s1z.at[y_at(d)], r2y, y_rs, ys_s, y_dev)
        dwst[...] = total_of(NY, s1z[y], r2y, y_rs)
        for copy in first_z(False) + second:
            copy.wait_send()

    @pl.when(c == 1)
    def _():
        acc = total_of(NY, wpart[:, y], r1y, y_rs)
        s1y[...] = acc.astype(jnp.bfloat16)
        second = fan(NZ, lambda d: s1y.at[z_at(d)], r2z, z_rs, zs_s, z_dev)
        dwst[...] = total_of(NZ, s1y[z], r2z, z_rs)
        for copy in first_y(False) + second:
            copy.wait_send()

    store(dwst, dw_hbm)
    for k in range(2):
        arrived(rretk.at[k], ret_rs.at[2 + k])
    key_total = dkacc[4] + rretk[0].astype(jnp.float32) + rretk[1].astype(jnp.float32)
    kg[...] = (key_total * HD ** (-0.5)).astype(jnp.bfloat16)
    store(kg, dk_hbm)
    for copy in sends:
        copy.wait_send()
    for copy in outs:
        copy.wait()


def shards(queries, keys, values, log_sums, out_grad, chosen, inputs):
    b16, f32 = jnp.bfloat16, jnp.float32
    any_ = pl.BlockSpec(memory_space=pl.ANY)
    sem = pltpu.SemaphoreType.DMA
    return pl.pallas_call(
        kernel,
        out_shape=(
            jax.ShapeDtypeStruct((T, G * HD), b16),
            jax.ShapeDtypeStruct((T, HD), b16),
            jax.ShapeDtypeStruct((T, HD), b16),
            jax.ShapeDtypeStruct((RW, HD), f32),
        ),
        in_specs=[any_] * 5 + [pl.BlockSpec(memory_space=pltpu.SMEM), any_],
        out_specs=(any_,) * 4,
        scratch_shapes=[
            pltpu.VMEM((G, T, HD), b16),
            pltpu.VMEM((G, T, HD), b16),
            pltpu.VMEM((G, T, HD), b16),
            pltpu.VMEM((G, T), f32),
            pltpu.VMEM((6, T, HD), b16),
            pltpu.VMEM((6, T, HD), b16),
            pltpu.VMEM((24, T), f32),
            pltpu.VMEM((NB, BL, T), f32),
            pltpu.VMEM((5, G, T, T), f32),
            pltpu.VMEM((5, T, T), f32),
            pltpu.VMEM((5, T, HD), f32),
            pltpu.VMEM((5, T, HD), f32),
            pltpu.VMEM((G, T, HD), b16),
            pltpu.VMEM((2, HR, T), b16),
            pltpu.VMEM((4, 2, HR, T), b16),
            pltpu.VMEM((2, T, HD), b16),
            pltpu.VMEM((2, T, HD), b16),
            pltpu.VMEM((2, T, HD), b16),
            pltpu.VMEM((2, T, HD), b16),
            pltpu.VMEM((2, T, HD), b16),
            pltpu.VMEM((2, T, HD), b16),
            pltpu.VMEM((2, T, HD), b16),
            pltpu.VMEM((2, T, HD), b16),
            pltpu.VMEM((2, T, HD), b16),
            pltpu.VMEM((T, HD), b16),
            pltpu.VMEM((NZ, NY, RW, HD), b16),
            pltpu.VMEM((NZ, NY, RW, HD), b16),
            pltpu.VMEM((NY, NZ, RW, HD), b16),
            pltpu.VMEM((NY, RW, HD), b16),
            pltpu.VMEM((NZ, RW, HD), b16),
            pltpu.VMEM((NZ, RW, HD), b16),
            pltpu.VMEM((NY, RW, HD), b16),
            pltpu.VMEM((RW, HD), f32),
            sem((21,)),
            sem((32,)),
            sem((6,)),
            sem((6,)),
            sem((4, 2)),
            sem((2,)),
            sem((4,)),
            sem,
            sem((NZ,)),
            sem((NY,)),
            sem((NZ,)),
            sem((NY,)),
            sem((10,)),
        ],
        compiler_params=pltpu.CompilerParams(
            collective_id=0, has_side_effects=True, vmem_limit_bytes=60 * 1024 * 1024
        ),
        name="step",
    )(queries, keys, values, log_sums, out_grad, chosen, inputs)


def solution(mesh):
    return jax.shard_map(
        shards,
        mesh=mesh,
        in_specs=(
            P("kv", "tp"),
            P("kv", "tp"),
            P("kv", "tp"),
            P("tp", "kv"),
            P("kv", "tp"),
            P("kv", "tp", None),
            P("kv", "tp"),
        ),
        out_specs=(P("kv", "tp"), P("kv", "tp"), P("kv", "tp"), P("kv", "tp")),
        check_vma=False,
    )
```

```python
import functools

import jax
import jax.numpy as jnp
from jax import lax
from jax.experimental import pallas as pl
from jax.experimental.pallas import tpu as pltpu
from jax.sharding import PartitionSpec as P

MESH = pl.DeviceIdType.MESH
LOG2E = 1.4426950408889634
MASKED = -1e30

NX, NY, NZ = 4, 8, 12
NCHIP = NY * NZ
T = 256
HD = 128
G = 6
BL = 64
NB = 4
SELS = 8
CPX = NCHIP // NX
RW = 16
HR = CPX * RW

NN = (((1,), (0,)), ((), ()))
NT = (((1,), (1,)), ((), ()))
TN = (((0,), (0,)), ((), ()))


def mm(a, b, dims):
    return lax.dot_general(a, b, dims, preferred_element_type=jnp.float32)


def kernel(
    q_hbm, k_hbm, v_hbm, lse_hbm, do_hbm, ch_hbm, in_hbm,
    dq_ref, dk_ref, dv_ref, dw_ref,
    ch_ref, q6, do6, in6, lse, kbuf, vbuf, hitb, ownb, pst, plow, dpst, dvacc, dkacc,
    hs, ing, sxv, rxv, sretv, rretv, sxk, rxk, sretk, rretk, vg,
    wpart, r1z, r1y, s1z, s1y, r2z, r2y,
    lsem, ssem, k_rs, v_rs, in_rs, x_rs, ret_rs, vg_rs, z_rs, y_rs, zs_s, ys_s, zk, yk,
):
    kv = lax.axis_index("kv")
    x = lax.axis_index("tp")
    p = kv // 2
    c = kv % 2
    z = p // NY
    y = p % NY
    o = 1 - c

    def wrapped(i, n):
        i = jnp.where(i >= n, i - n, i)
        return jnp.where(i < 0, i + n, i)

    def chip(step):
        return wrapped(p + step, NCHIP)

    def at(chip_id, core):
        return (chip_id * 2 + core, x)

    partner = at(p, o)
    nxt, prv, prv2, nxt2 = (at(chip(s), c) for s in (1, -1, -2, 2))
    xr, xl = wrapped(x + 1, NX), wrapped(x - 1, NX)

    def z_at(d):
        return wrapped(z + d, NZ)

    def y_at(d):
        return wrapped(y + d, NY)

    def z_dev(d):
        return at(z_at(d) * NY + y, c)

    def y_dev(d):
        return at(z * NY + y_at(d), c)

    loads = []

    def load(src, dst, n):
        copy = pltpu.make_async_copy(src, dst, lsem.at[n])
        copy.start()
        return copy

    ld_k = load(k_hbm, kbuf.at[4 + c], 0)
    ld_c = load(ch_hbm, ch_ref, 21)

    barrier = pltpu.get_barrier_semaphore()
    peers = [partner, nxt, nxt2, prv, prv2]
    peers += [(p * 2 + d, xx) for xx in (xr, xl) for d in (0, 1)]
    peers += [z_dev(1), z_dev(-1), y_dev(1), y_dev(-1)]
    for peer in peers:
        pl.semaphore_signal(barrier, inc=1, device_id=peer, device_id_type=MESH)

    def tell(k):
        for sem, dev, top in ((zk, z_dev, 3), (yk, y_dev, 2)):
            if k < top:
                for d in (1 << k, -(1 << k)):
                    pl.semaphore_signal(sem.at[k], inc=1, device_id=dev(d), device_id_type=MESH)

    def told(k):
        for sem, top in ((zk, 3), (yk, 2)):
            if k < top:
                with jax.named_scope(f"told{k}"):
                    pl.semaphore_wait(sem.at[k], 2)

    sends = []

    def send(src, dst, recv, device):
        n = len(sends)
        copy = pltpu.make_async_remote_copy(
            src_ref=src, dst_ref=dst, send_sem=ssem.at[n], recv_sem=recv,
            device_id=device, device_id_type=MESH,
        )
        copy.start()
        sends.append(copy)
        return copy

    waits = []

    def arrived(dst, recv):
        waits.append(0)
        with jax.named_scope(f'w{len(waits)}'):
            pltpu.make_async_copy(dst, dst, recv).wait()

    def kv_send(buf, rs, slot, device):
        send(buf.at[slot], buf.at[slot], rs.at[slot], device)

    def kv_send_to(buf, rs, src_slot, dst_slot, device):
        send(buf.at[src_slot], buf.at[dst_slot], rs.at[dst_slot], device)

    def half_of(slot, i):
        return kbuf.at[slot, pl.ds(i * (T // 2), T // 2)]

    def k_send(src_slot, dst_slot, i, device):
        send(half_of(src_slot, i), half_of(dst_slot, i), k_rs.at[dst_slot, i], device)

    def k_arrived(slot, i):
        arrived(half_of(slot, i), k_rs.at[slot, i])

    ld_k.wait()
    with jax.named_scope("w_barrier"):
        pl.semaphore_wait(barrier, len(peers))

    for i in (0, 1):
        k_send(4 + c, 2 + c, i, nxt)
    for i in (0, 1):
        k_send(4 + c, 4 + c, i, partner)
    ld_v = load(v_hbm, vbuf.at[4 + c], 8)
    ld_i = [load(in_hbm.at[:, pl.ds(HD * h, HD)], in6.at[h], 9 + h) for h in range(G)]
    ld_q = [load(q_hbm.at[:, pl.ds(HD * h, HD)], q6.at[h], 1 + h) for h in range(G)]
    ld_l = load(lse_hbm, lse, 7)
    ld_d = [load(do_hbm.at[:, pl.ds(HD * h, HD)], do6.at[h], 15 + h) for h in range(G)]
    ld_v.wait()
    kv_send_to(vbuf, v_rs, 4 + c, 2 + c, nxt)
    kv_send(vbuf, v_rs, 4 + c, partner)

    for j in range(G):
        ld_i[j].wait()
        xt = in6[j].T
        for m in range(4):
            for d in range(2):
                r0 = (4 * j + m) * RW
                hs[d, r0 : r0 + RW, :] = xt[32 * m + 16 * d : 32 * m + 16 * d + 16, :]

    send(hs.at[o], ing.at[0, c], in_rs.at[0, c], partner)
    def inputs_out(side_of_core):
        side = jnp.where(side_of_core == 0, xr, xl)
        rel = jnp.where(side_of_core == 0, 3, 1)
        for d in (0, 1):
            send(hs.at[d], ing.at[rel, c], in_rs.at[rel, c], (p * 2 + d, side))

    inputs_out(c)

    ld_c.wait()
    base = (p - 2) * 4 * 2 + 4 * c
    own0 = kv * NB
    wid = lax.broadcasted_iota(jnp.int32, (24, T), 0)
    lane = lax.broadcasted_iota(jnp.int32, (24, T), 1)
    hit = jnp.zeros((24, T), jnp.float32)
    for b in range(NB):
        in_b = (lane // BL) == b
        for k in range(SELS):
            named = ch_ref[b, 0, k]
            slot = jnp.where(named < own0 + b, named - base, -1)
            hit = jnp.where(in_b & (wid == slot), 1.0, hit)
    hitb[...] = jnp.where(hit > 0.5, 0.0, MASKED)
    krow = lax.broadcasted_iota(jnp.int32, (BL, T), 0)
    qlane = lax.broadcasted_iota(jnp.int32, (BL, T), 1)
    for j in range(NB):
        here = (qlane // BL) == j
        causal = here & (krow <= qlane - BL * j)
        ownb[j] = jnp.where(causal, 0.0, jnp.where(here, MASKED, hitb[16 + j : 17 + j, :]))

    for copy in ld_q:
        copy.wait()
    ld_l.wait()
    for copy in ld_d:
        copy.wait()

    lse[...] = lse[...] * LOG2E
    factor = HD ** (-0.5) * LOG2E

    def value_terms(s):
        with jax.named_scope(f"value_terms{s}"):
            keys = kbuf[s + c]
            for h in range(G):
                scores = mm(keys, q6[h], NT)
                row = lse[h : h + 1, :]
                for j in range(NB):
                    part = scores[BL * j : BL * j + BL, :] * factor
                    if s == 4:
                        shift = ownb[j] - row
                    else:
                        shift = hitb[4 * s + j : 4 * s + j + 1, :] - row
                    part = jnp.exp2(part + shift)
                    pst[s, h, BL * j : BL * j + BL, :] = part
                    plow[s, BL * j : BL * j + BL, T * h : T * h + T] = part.astype(jnp.bfloat16)
            half = G // 2
            dvacc[s] = mm(
                plow[s, :, : T * half], do6[:half].reshape(T * half, HD), NN
            ) + mm(plow[s, :, T * half :], do6[half:].reshape(T * half, HD), NN)

    tell(0)
    value_terms(4)
    for i in (0, 1):
        k_arrived(2 + c, i)
        k_send(2 + c, c, i, nxt)
        k_send(2 + c, 2 + c, i, partner)
    value_terms(2)
    arrived(vbuf.at[2 + c], v_rs.at[2 + c])
    kv_send_to(vbuf, v_rs, 2 + c, c, nxt)
    kv_send(vbuf, v_rs, 2 + c, partner)
    for slot in (2 + o, 4 + o):
        for i in (0, 1):
            k_arrived(slot, i)
    inputs_out(o)
    value_terms(3)
    for i in (0, 1):
        k_arrived(c, i)
        k_send(c, c, i, partner)
    value_terms(0)
    for i in (0, 1):
        k_arrived(o, i)
    value_terms(1)

    sxv[0] = dvacc[1].astype(jnp.bfloat16)
    sxv[1] = dvacc[3].astype(jnp.bfloat16)
    send(sxv, rxv, x_rs.at[0], partner)
    arrived(ing.at[3, 0], in_rs.at[3, 0])
    send(ing.at[3, 0], ing.at[2, 0], in_rs.at[2, 0], (kv, xr))
    arrived(ing.at[1, 1], in_rs.at[1, 1])
    send(ing.at[1, 1], ing.at[2, 1], in_rs.at[2, 1], (kv, xl))
    told(0)
    tell(1)

    def score_terms(h):
        with jax.named_scope(f"score_terms{h}"):
            delta = jnp.zeros((1, T), jnp.float32)
            for s in range(5):
                dp = mm(vbuf[s + c], do6[h], NT)
                dpst[h % 2, s] = dp
                delta = delta + jnp.sum(pst[s, h] * dp, axis=0, keepdims=True)
            dqt = jnp.zeros((HD, T), jnp.float32)
            for s in range(5):
                ds = (pst[s, h] * (dpst[h % 2, s] - delta)).astype(jnp.bfloat16)
                if h == 0:
                    dkacc[s] = mm(ds, q6[h], NN)
                else:
                    dkacc[s] += mm(ds, q6[h], NN)
                dqt = dqt + mm(kbuf[s + c], ds, TN)
            dq_ref[:, HD * h : HD * h + HD] = (dqt * HD ** (-0.5)).T.astype(jnp.bfloat16)

    arrived(vbuf.at[c], v_rs.at[c])
    kv_send(vbuf, v_rs, c, partner)

    arrived(rxv, x_rs.at[0])
    for k in range(2):
        dvacc[2 * k + 2 * o] += rxv[k].astype(jnp.float32)
    sretv[0] = dvacc[0].astype(jnp.bfloat16)
    sretv[1] = dvacc[2].astype(jnp.bfloat16)
    send(sretv.at[0], rretv.at[0], ret_rs.at[0], prv2)
    send(sretv.at[1], rretv.at[1], ret_rs.at[1], prv)

    for slot in (2 + o, 4 + o, o):
        arrived(vbuf.at[slot], v_rs.at[slot])
    score_terms(0)
    score_terms(1)
    told(1)
    tell(2)
    score_terms(2)
    score_terms(3)

    for k in range(2):
        arrived(rretv.at[k], ret_rs.at[k])
    total = dvacc[4] + rretv[0].astype(jnp.float32) + rretv[1].astype(jnp.float32)
    vg[c] = total.astype(jnp.bfloat16)
    send(vg.at[c], vg.at[c], vg_rs, partner)
    dv_ref[...] = vg[c]
    score_terms(4)
    told(2)

    arrived(ing.at[0, o], in_rs.at[0, o])
    arrived(ing.at[3, 1], in_rs.at[3, 1])
    arrived(ing.at[1, 0], in_rs.at[1, 0])
    for d in (0, 1):
        arrived(ing.at[2, d], in_rs.at[2, d])
    arrived(vg.at[o], vg_rs)

    for rel in range(4):
        if rel == 0:
            rows = mm(hs[c], vg[c], NN) + mm(ing[0, o], vg[o], NN)
        else:
            rows = mm(ing[rel, 0], vg[0], NN) + mm(ing[rel, 1], vg[1], NN)
        first = wrapped(x + rel, NX) * (CPX // NY)
        tiles = rows.astype(jnp.bfloat16).reshape(CPX, RW, HD)
        for a in range(CPX // NY):
            wpart[first + a] = tiles[a * NY : (a + 1) * NY]

    def fan(n, src, dst, recv, sem, device, start=True):
        copies = []
        for d in range(1, n):
            copy = pltpu.make_async_remote_copy(
                src_ref=src(d), dst_ref=dst.at[d], send_sem=sem.at[d], recv_sem=recv.at[d],
                device_id=device(d), device_id_type=MESH,
            )
            if start:
                copy.start()
            copies.append(copy)
        return copies

    def total_of(n, own, got, recv):
        acc = own.astype(jnp.float32)
        for d in range(1, n):
            arrived(got.at[d], recv.at[d])
            acc = acc + got[d].astype(jnp.float32)
        return acc

    def first_z(start):
        return fan(NZ, lambda d: wpart.at[z_at(d)], r1z, z_rs, zs_s, z_dev, start)

    def first_y(start):
        return fan(NY, lambda d: wpart.at[:, y_at(d)], r1y, y_rs, ys_s, y_dev, start)

    @pl.when(c == 1)
    def _():
        first_z(True)

    @pl.when(c == 0)
    def _():
        first_y(True)

    score_terms(5)
    sxk[0] = dkacc[1].astype(jnp.bfloat16)
    sxk[1] = dkacc[3].astype(jnp.bfloat16)
    send(sxk, rxk, x_rs.at[1], partner)
    arrived(rxk, x_rs.at[1])
    for k in range(2):
        dkacc[2 * k + 2 * o] += rxk[k].astype(jnp.float32)
    sretk[0] = dkacc[0].astype(jnp.bfloat16)
    send(sretk.at[0], rretk.at[0], ret_rs.at[2], prv)

    def second_y(start):
        return fan(NY, lambda d: s1z.at[y_at(d)], r2y, y_rs, ys_s, y_dev, start)

    def second_z(start):
        return fan(NZ, lambda d: s1y.at[z_at(d)], r2z, z_rs, zs_s, z_dev, start)

    @pl.when(c == 1)
    def _():
        s1z[...] = total_of(NZ, wpart[z], r1z, z_rs).astype(jnp.bfloat16)
        second_y(True)

    @pl.when(c == 0)
    def _():
        s1y[...] = total_of(NY, wpart[:, y], r1y, y_rs).astype(jnp.bfloat16)
        second_z(True)

    arrived(rretk.at[0], ret_rs.at[2])
    sretk[1] = (dkacc[2] + rretk[0].astype(jnp.float32)).astype(jnp.bfloat16)
    send(sretk.at[1], rretk.at[1], ret_rs.at[3], prv)

    @pl.when(c == 1)
    def _():
        dw_ref[...] = total_of(NY, s1z[y], r2y, y_rs)
        for copy in first_z(False) + second_y(False):
            copy.wait_send()

    @pl.when(c == 0)
    def _():
        dw_ref[...] = total_of(NZ, s1y[z], r2z, z_rs)
        for copy in first_y(False) + second_z(False):
            copy.wait_send()

    arrived(rretk.at[1], ret_rs.at[3])
    key_total = dkacc[4] + rretk[1].astype(jnp.float32)
    dk_ref[...] = (key_total * HD ** (-0.5)).astype(jnp.bfloat16)
    for copy in sends:
        copy.wait_send()


def put_out(*refs):
    n = len(refs) // 2
    sems = refs[-1]
    copies = [pltpu.make_async_copy(refs[i], refs[n + i], sems.at[i]) for i in range(n)]
    for copy in copies:
        copy.start()
    for copy in copies:
        copy.wait()


def shards(queries, keys, values, log_sums, out_grad, chosen, inputs):
    b16, f32 = jnp.bfloat16, jnp.float32
    any_ = pl.BlockSpec(memory_space=pl.ANY)
    sem = pltpu.SemaphoreType.DMA
    results = pl.pallas_call(
        kernel,
        out_shape=(
            pltpu.VMEM((T, G * HD), b16),
            pltpu.VMEM((T, HD), b16),
            pltpu.VMEM((T, HD), b16),
            pltpu.VMEM((RW, HD), f32),
        ),
        in_specs=[any_] * 7,
        out_specs=(pl.BlockSpec(memory_space=pltpu.VMEM),) * 4,
        scratch_shapes=[
            pltpu.SMEM((NB, 1, SELS), jnp.int32),
            pltpu.VMEM((G, T, HD), b16),
            pltpu.VMEM((G, T, HD), b16),
            pltpu.VMEM((G, T, HD), b16),
            pltpu.VMEM((G, T), f32),
            pltpu.VMEM((6, T, HD), b16),
            pltpu.VMEM((6, T, HD), b16),
            pltpu.VMEM((24, T), f32),
            pltpu.VMEM((NB, BL, T), f32),
            pltpu.VMEM((5, G, T, T), f32),
            pltpu.VMEM((5, T, G * T), b16),
            pltpu.VMEM((2, 5, T, T), f32),
            pltpu.VMEM((5, T, HD), f32),
            pltpu.VMEM((5, T, HD), f32),
            pltpu.VMEM((2, HR, T), b16),
            pltpu.VMEM((4, 2, HR, T), b16),
            pltpu.VMEM((2, T, HD), b16),
            pltpu.VMEM((2, T, HD), b16),
            pltpu.VMEM((2, T, HD), b16),
            pltpu.VMEM((2, T, HD), b16),
            pltpu.VMEM((2, T, HD), b16),
            pltpu.VMEM((2, T, HD), b16),
            pltpu.VMEM((2, T, HD), b16),
            pltpu.VMEM((2, T, HD), b16),
            pltpu.VMEM((2, T, HD), b16),
            pltpu.VMEM((NZ, NY, RW, HD), b16),
            pltpu.VMEM((NZ, NY, RW, HD), b16),
            pltpu.VMEM((NY, NZ, RW, HD), b16),
            pltpu.VMEM((NY, RW, HD), b16),
            pltpu.VMEM((NZ, RW, HD), b16),
            pltpu.VMEM((NZ, RW, HD), b16),
            pltpu.VMEM((NY, RW, HD), b16),
            sem((22,)),
            sem((48,)),
            sem((6, 2)),
            sem((6,)),
            sem((4, 2)),
            sem((2,)),
            sem((4,)),
            sem,
            sem((NZ,)),
            sem((NY,)),
            sem((NZ,)),
            sem((NY,)),
            pltpu.SemaphoreType.REGULAR((3,)),
            pltpu.SemaphoreType.REGULAR((2,)),
        ],
        compiler_params=pltpu.CompilerParams(
            collective_id=0, has_side_effects=True, vmem_limit_bytes=66450000
        ),
        name="step",
    )(queries, keys, values, log_sums, out_grad, chosen, inputs)
    return pl.pallas_call(
        put_out,
        out_shape=tuple(jax.ShapeDtypeStruct(r.shape, r.dtype) for r in results),
        in_specs=[pl.BlockSpec(memory_space=pltpu.VMEM)] * 4,
        out_specs=(any_,) * 4,
        scratch_shapes=[sem((4,))],
        compiler_params=pltpu.CompilerParams(vmem_limit_bytes=1 << 20),
        name="put_out",
    )(*results)


def solution(mesh):
    return jax.shard_map(
        shards,
        mesh=mesh,
        in_specs=(
            P("kv", "tp"),
            P("kv", "tp"),
            P("kv", "tp"),
            P("tp", "kv"),
            P("kv", "tp"),
            P("kv", "tp", None),
            P("kv", "tp"),
        ),
        out_specs=(P("kv", "tp"), P("kv", "tp"), P("kv", "tp"), P("kv", "tp")),
        check_vma=False,
    )
```
